32 devices in a mesh: ep: 4 (over y, x), tp: 8 (over z, core).
Axes of the slice: x: 2, y: 2, z: 4, core: 2. Of those that a mesh axis runs over, the one named last changes fastest.
Arguments:
- mixer_input_channels: bfloat16 [8192, 2048], P('ep', 'tp'), may hold values from -6 to 6
- output_gate_logits: bfloat16 [8192, 2048], P('ep', 'tp'), may hold values from -6 to 6
- head_group_input_map: bfloat16 [8192, 256], P('ep'), may hold values from -6 to 6
- head_group_output_map: bfloat16 [8192, 256], P('ep'), may hold values from -6 to 6
- input_channel_taps: bfloat16 [4, 2048], P(None, 'tp'), may hold values from -3 to 3
- input_map_taps: bfloat16 [4, 256], replicated, may hold values from -3 to 3
- output_map_taps: bfloat16 [4, 256], replicated, may hold values from -3 to 3
- step_logits: float32 [32, 8192], P('tp', 'ep'), may hold values from -5 to 5
- head_log_rate: float32 [32], P('tp'), may hold values from -20 to -2
- extra_log_decay: float32 [32, 8192], P('tp', 'ep'), may hold values from -1 to 0
- head_direct_scale: float32 [32], P('tp'), may hold values from 1 to 6
- gated_norm_scale: bfloat16 [2048], P('tp'), may hold values from 0.099609375 to 1.8984375
- mixer_output_weight: bfloat16 [2048, 2048], P('tp'), may hold values from -0.125 to 0.125
- second_batch_tokens: bfloat16 [1024, 2048], P('ep'), may hold values from -6 to 6
- pre_expert_norm_scale: bfloat16 [2048], replicated, may hold values from 0.099609375 to 1.8984375
- group_router_columns: bfloat16 [2048, 1], replicated
- expert_router_columns: bfloat16 [2048, 4], replicated
- routes: int32 [1024, 2], P('ep'), may hold values from 0 to 3, all different within a row; in each aligned block of 256 rows (0 to 255, 256 to 511, ...) at most 256 rows name the same one
- expert_gate_weight: bfloat16 [4, 2048, 4096], P('ep', None, 'tp'), may hold values from -0.125 to 0.125
- expert_up_weight: bfloat16 [4, 2048, 4096], P('ep', None, 'tp'), may hold values from -0.125 to 0.125
- expert_down_weight: bfloat16 [4, 4096, 2048], P('ep', 'tp'), may hold values from -0.125 to 0.125
Outputs:
- mixer_out: bfloat16 [8192, 2048], P(('ep', 'tp'))
- experts_out: bfloat16 [1024, 2048], P('ep', 'tp')
The draws below stay inside these ranges and needn't reach their ends.
Inputs may be any that keep to these rules, and one draw needn't show every extreme that they name: `routes`: in each aligned block of 256 rows no expert is named more than 256 times, some expert exactly 256 times in some block; a row's two experts differ.
All inputs are finite; a program needn't handle non-finite values.
Results may differ from the reference program's by a relative error of at most 0.019.
Values may be sent and summed in bfloat16 or wider, within the bound.
No kernel may reach another device: no remote copies, remote signals or barrier semaphores. Data moves between devices by JAX's collectives and lax.ppermute only.
A program may use at most 128 MiB of HBM per device.

```python
import math
import jax
import jax.numpy as jnp
import numpy as np
from jax import lax

D = 2048
HEADS = 32
HEAD_DIM = 64
STATE = 64
GROUPS = 4
CONV = 4
BLOCK = 128
FF = 4096
TOK_SHARD = 2048
TOKB = 256
INNER = 2048
SEQ = 8192
TOKENS = 1024
EXPERTS = 4
EXPERT_GROUPS = 1
CAP = 256
FF_SHARD = 512
N_EP = 4
N_TP = 8


def draw_step_logits(key, part):
    first, second = jax.random.split(jax.random.fold_in(key, 11))
    span = max(TOK_SHARD // 2, 1)
    offset = jax.random.uniform(second, (HEADS, SEQ // span), jnp.float32, -1.5, 1.5)
    offset = jnp.repeat(offset, span, axis=1)
    noise = jnp.clip(jax.random.normal(first, (HEADS, SEQ), jnp.float32), -3.0, 3.0)
    return (noise + offset).astype(jnp.float32)


def draw_head_log_rate(key, part):
    first, second, third = jax.random.split(jax.random.fold_in(key, 12), 3)
    share = 0.5
    quick = jax.random.uniform(first, (HEADS,), jnp.float32) < share
    quick_rate = jax.random.uniform(second, (HEADS,), jnp.float32, math.log(0.02), math.log(0.1))
    slow_rate = jax.random.uniform(third, (HEADS,), jnp.float32, math.log(0.3), math.log(2.3)) - math.log(SEQ)
    return jnp.where(quick, quick_rate, slow_rate).astype(jnp.float32)


def draw_extra_log_decay(key, part):
    first, second = jax.random.split(jax.random.fold_in(key, 13))
    struck = jax.random.uniform(first, (HEADS, SEQ), jnp.float32) < 6.0 / SEQ
    depth = jax.random.uniform(second, (HEADS, SEQ), jnp.float32, math.log(0.5), math.log(0.8))
    return jnp.where(struck, depth, 0.0).astype(jnp.float32)


def router_columns(key, columns):
    first = jax.random.fold_in(key, 0)
    base = jax.random.normal(first, (D, columns), jnp.float32) / math.sqrt(D)
    return base.astype(jnp.bfloat16)


def draw_group_router_columns(key, part):
    return router_columns(jax.random.fold_in(key, 14), EXPERT_GROUPS)


def draw_expert_router_columns(key, part):
    return router_columns(jax.random.fold_in(key, 15), EXPERTS)


def spiked(result, stream_key, source, target, shards_of, factor):
    owner, partner = [(jnp.arange(result.shape[position]) // (result.shape[position] // shards_of)).reshape([-1 if axis == position else 1 for axis in range(result.ndim)]) for position in (source, target)]
    chosen = jax.random.permutation(stream_key, shards_of)[partner]
    strong = (owner == chosen) | (owner == (partner + shards_of // 2) % shards_of)
    return jnp.where(strong, factor * result, result)


def block_levels(stream_key, extent, cuts, low, high):
    def one(axis_at, blocks):
        draws = jax.random.uniform(jax.random.fold_in(jax.random.fold_in(stream_key, 6), axis_at), (blocks,), jnp.float32, low / len(cuts), high / len(cuts))
        return jnp.repeat(jnp.exp(draws), extent[axis_at] // blocks).reshape((-1,) + (1,) * (len(extent) - axis_at - 1))

    gain = one(*cuts[0])
    for cut in cuts[1:]:
        gain = gain * one(*cut)
    return gain


def deal_out(stream_key, own, number, rows, amount, top, bound, skew):
    order = jax.random.permutation(stream_key, amount)
    packed, common = load_shares(amount, rows * top, bound, skew, True), load_shares(amount, rows * top, bound, skew, False)
    places = jnp.arange(amount)

    def named(sizes, turn):
        used = int((sizes > 0).sum())
        fixed = max(1, used // 4)
        moved = fixed + (places - fixed + turn * (used - fixed)) % max(1, amount - fixed)
        return jnp.zeros((amount,), jnp.int32).at[order[jnp.where(places < fixed, places, moved)]].set(jnp.asarray(sizes, jnp.int32))

    sizes = jnp.where(number % 4 == 0, named(packed, number // 4), named(common, number - number // 4 - 1))
    mixed = jax.random.permutation(jax.random.fold_in(own, 3), amount)
    donor, taker = mixed[0:amount // 2 * 2:2], mixed[1:amount // 2 * 2:2]
    margin = jnp.minimum(sizes[donor] - 1, bound - sizes[taker]) // 2
    margin = jnp.where((donor == order[0]) | (taker == order[0]) | (sizes[taker] == 0), 0, jnp.maximum(margin, 0))
    moved = jax.random.randint(jax.random.fold_in(own, 4), (amount // 2,), 0, 1 << 20) % (margin + 1)
    sizes = sizes.at[donor].add(-moved).at[taker].add(moved)
    members = jnp.searchsorted(jnp.cumsum(sizes), jnp.arange(rows * top), side="right").astype(jnp.int32)
    grid = members.reshape(top, rows).T
    grid = grid[jax.random.permutation(jax.random.fold_in(own, 1), rows)]
    turn = jax.random.randint(jax.random.fold_in(own, 2), (rows, 1), 0, top)
    return jnp.take_along_axis(grid, (jnp.arange(top)[None, :] + turn) % top, axis=1)


def load_shares(number_of, total, limit, skew, full):
    loads = [(1 << 20) // math.isqrt(rank ** skew) + 1 for rank in range(1, number_of + 1)]
    largest = limit if full else min(limit, max(-(-total // number_of), total * loads[0] // sum(loads)))
    least = 1 if total - largest >= number_of - 1 else 0
    given, spare = [largest] + [least] * (number_of - 1), total - largest - least * (number_of - 1)
    while spare > 0:
        free = [i for i in range(1, number_of) if given[i] < largest] or [i for i in range(1, number_of) if given[i] < limit]
        whole, left = sum([loads[i] for i in free]), spare
        for i in free:
            more = min(limit - given[i], max(1, left * loads[i] // whole), spare)
            given[i] = given[i] + more
            spare = spare - more
    return np.array(given)


def bell_draw(key, shape, spread, most, cuts=(), kind=jnp.bfloat16):
    entries = jax.random.normal(key, shape, jnp.float32) * spread
    if len(cuts) > 0:
        entries = block_levels(key, shape, cuts, -0.22, 0.18) * entries
    return jnp.clip(entries, min=-most, max=most).astype(kind)


def noise_with(key, extent, deviation, reach, shards, heavy, kind=jnp.bfloat16):
    result = deviation * jax.random.normal(key, extent, jnp.float32)
    if shards:
        result = result * block_levels(key, extent, shards, -0.22, 0.18)
    return jnp.clip(spiked(result, jax.random.fold_in(key, 3), *heavy), -reach, reach).astype(kind)


def setup_inputs(seed: int = 0) -> dict:
    splits = jax.random.split(jax.random.key(seed), 22)
    mixer_input_channels = bell_draw(splits[0], (SEQ, INNER), 1.0, 6.0, ((0, 4), (1, 8)))
    output_gate_logits = bell_draw(splits[1], (SEQ, INNER), 1.0, 6.0, ((0, 4), (1, 8)))
    head_group_input_map = bell_draw(splits[2], (SEQ, GROUPS * STATE), 1.0, 6.0, ((0, 4),))
    head_group_output_map = bell_draw(splits[3], (SEQ, GROUPS * STATE), 1.0, 6.0, ((0, 4),))
    input_channel_taps = bell_draw(splits[4], (CONV, INNER), CONV ** -0.5, 3.0, ((1, 8),))
    input_map_taps = bell_draw(splits[5], (CONV, GROUPS * STATE), CONV ** -0.5, 3.0)
    output_map_taps = bell_draw(splits[6], (CONV, GROUPS * STATE), CONV ** -0.5, 3.0)
    step_logits = draw_step_logits(jax.random.fold_in(splits[21], 71), 0)
    head_log_rate = draw_head_log_rate(jax.random.fold_in(splits[21], 71), 0)
    extra_log_decay = draw_extra_log_decay(jax.random.fold_in(splits[21], 71), 0)
    head_direct_scale = jnp.clip(1.0 + 5.0 * jax.random.uniform(splits[10], (HEADS,), jnp.float32) ** block_levels(splits[10], (HEADS,), ((0, 8),), -0.2, 0.2), 1.0, 6.0)
    gated_norm_scale = jnp.clip(1.0 + 0.18 * jax.random.normal(splits[11], (INNER,), jnp.float32), 0.099609375, 1.8984375).astype(jnp.bfloat16)
    mixer_output_weight = bell_draw(splits[12], (INNER, D), INNER ** -0.5, 0.125, ((0, 8),))
    second_batch_tokens = bell_draw(splits[13], (TOKENS, D), 1.0, 6.0, ((0, 4),))
    pre_expert_norm_scale = jnp.clip(1.0 + 0.18 * jax.random.normal(splits[14], (D,), jnp.float32), 0.099609375, 1.8984375).astype(jnp.bfloat16)
    group_router_columns = draw_group_router_columns(jax.random.fold_in(splits[21], 71), 0)
    expert_router_columns = draw_expert_router_columns(jax.random.fold_in(splits[21], 71), 0)
    routes_keys = jax.random.split(jax.random.fold_in(splits[17], 1), TOKENS // TOKB)
    routes_turns = jax.random.permutation(jax.random.fold_in(splits[17], 3), TOKENS // TOKB)
    routes = jax.vmap(lambda own, number: deal_out(jax.random.fold_in(splits[17], 2), own, number, TOKB, EXPERTS, 2, CAP, 2))(routes_keys, routes_turns).reshape((TOKENS, 2))
    expert_gate_weight = bell_draw(splits[18], (EXPERTS, D, FF), D ** -0.5, 0.125, ((0, 4), (2, 8)))
    expert_up_weight = bell_draw(splits[19], (EXPERTS, D, FF), D ** -0.5, 0.125, ((0, 4), (2, 8)))
    expert_down_weight = noise_with(splits[20], (EXPERTS, FF, D), FF ** -0.5, 0.125, ((0, 4), (1, 8)), (1, 2, 8, 2.0))
    return {"mixer_input_channels": mixer_input_channels, "output_gate_logits": output_gate_logits, "head_group_input_map": head_group_input_map, "head_group_output_map": head_group_output_map, "input_channel_taps": input_channel_taps, "input_map_taps": input_map_taps, "output_map_taps": output_map_taps, "step_logits": step_logits, "head_log_rate": head_log_rate, "extra_log_decay": extra_log_decay, "head_direct_scale": head_direct_scale, "gated_norm_scale": gated_norm_scale, "mixer_output_weight": mixer_output_weight, "second_batch_tokens": second_batch_tokens, "pre_expert_norm_scale": pre_expert_norm_scale, "group_router_columns": group_router_columns, "expert_router_columns": expert_router_columns, "routes": routes, "expert_gate_weight": expert_gate_weight, "expert_up_weight": expert_up_weight, "expert_down_weight": expert_down_weight}


eps = 1e-06
exact_prec = lax.Precision.HIGHEST

def causal_conv(joined, taps):
    width = taps.shape[0]
    length = joined.shape[0]
    padded = jnp.pad(joined.astype(jnp.float32), ((width - 1, 0), (0, 0)))
    total = jnp.zeros((length, joined.shape[1]), jnp.float32)
    for j in range(width):
        total = total + taps[j].astype(jnp.float32) * padded[j:j + length]
    return jax.nn.silu(total).astype(jnp.bfloat16)

def slot_positions(route_rows, n_experts):
    flat = route_rows.reshape(-1)
    onehot = (flat[:, None] == jnp.arange(n_experts, dtype=jnp.int32)[None, :]).astype(jnp.int32)
    return (lax.optimization_barrier(jnp.sum(onehot * jnp.cumsum(onehot, axis=0), axis=1)) - 1).astype(jnp.int32)

def route_weights(group_logits, expert_logits, routes):
    n_groups = group_logits.shape[1]
    n_experts = expert_logits.shape[1]
    per_group = n_experts // n_groups
    group_lp = jax.nn.log_softmax(group_logits, axis=-1)
    inner_lp = jax.nn.log_softmax(expert_logits.reshape(-1, n_groups, per_group), axis=-1).reshape(-1, n_experts)
    total = jnp.repeat(group_lp, per_group, axis=1) + inner_lp
    pick = routes[:, :, None] == jnp.arange(n_experts, dtype=jnp.int32)[None, None, :]
    chosen = lax.optimization_barrier(jnp.sum(jnp.where(pick, total[:, None, :], 0.0), axis=-1))
    return jax.nn.softmax(chosen, axis=-1)

def expert_apply(items):
    rows, gate_w, up_w, down_w = items
    gate = jnp.dot(rows, gate_w, preferred_element_type=jnp.float32)
    upper = jnp.dot(rows, up_w, preferred_element_type=jnp.float32)
    hidden = (jax.nn.silu(gate) * upper).astype(jnp.bfloat16)
    parts = hidden.reshape(rows.shape[0], N_TP, FF_SHARD).astype(jnp.float32)
    down_parts = down_w.reshape(N_TP, FF_SHARD, D).astype(jnp.float32)
    partial_sums = jnp.einsum('rjf,jfd->jrd', parts, down_parts).astype(jnp.bfloat16)
    return lax.optimization_barrier(jnp.sum(partial_sums.astype(jnp.float32), axis=0)).astype(jnp.bfloat16)

def reference(mixer_input_channels, output_gate_logits, head_group_input_map, head_group_output_map, input_channel_taps, input_map_taps, output_map_taps, step_logits, head_log_rate, extra_log_decay, head_direct_scale, gated_norm_scale, mixer_output_weight, second_batch_tokens, pre_expert_norm_scale, group_router_columns, expert_router_columns, routes, expert_gate_weight, expert_up_weight, expert_down_weight):
    joined = jnp.concatenate([mixer_input_channels, head_group_input_map, head_group_output_map], axis=1)
    taps = jnp.concatenate([input_channel_taps, input_map_taps, output_map_taps], axis=1)
    conv = causal_conv(joined, taps)
    xs = conv[:, :INNER]
    bs = conv[:, INNER:INNER + GROUPS * STATE]
    cs = conv[:, INNER + GROUPS * STATE:]
    time_step = jax.nn.softplus(step_logits)
    position_log_decay = extra_log_decay - time_step * jnp.exp(head_log_rate)[:, None]
    per_group = HEADS // GROUPS
    xs_f = xs.astype(jnp.float32).reshape(SEQ, HEADS, HEAD_DIM)
    x_dt = xs_f * jnp.transpose(time_step)[:, :, None]
    bs_h = jnp.repeat(bs.astype(jnp.float32).reshape(SEQ, GROUPS, STATE), per_group, axis=1)
    cs_h = jnp.repeat(cs.astype(jnp.float32).reshape(SEQ, GROUPS, STATE), per_group, axis=1)
    nblk = SEQ // BLOCK
    items = (x_dt.reshape(nblk, BLOCK, HEADS, HEAD_DIM), bs_h.reshape(nblk, BLOCK, HEADS, STATE), cs_h.reshape(nblk, BLOCK, HEADS, STATE), jnp.transpose(position_log_decay).reshape(nblk, BLOCK, HEADS))
    lower = jnp.tril(jnp.ones((BLOCK, BLOCK), bool))[:, :, None]

    def one_block(state, item):
        xb, bb, cb, lb = item
        cum = jnp.cumsum(lb, axis=0)
        diff = cum[:, None, :] - cum[None, :, :]
        weight = jnp.where(lower, jnp.exp(jnp.where(lower, diff, 0.0)), 0.0)
        scores = jnp.einsum('lhn,shn->lsh', cb, bb, precision=exact_prec)
        inner = jnp.einsum('lsh,shp->lhp', scores * weight, xb, precision=exact_prec)
        carried = jnp.einsum('lhn,hpn->lhp', cb, state, precision=exact_prec) * jnp.exp(cum)[:, :, None]
        tail = jnp.exp(cum[-1:] - cum)
        new_state = state * jnp.exp(cum[-1])[:, None, None] + jnp.einsum('shp,shn->hpn', xb * tail[:, :, None], bb, precision=exact_prec)
        return (new_state, inner + carried)
    start = jnp.zeros((HEADS, HEAD_DIM, STATE), jnp.float32)
    _, ssm = lax.scan(one_block, start, items)
    ssm = ssm.reshape(SEQ, HEADS, HEAD_DIM)
    gated = (ssm + head_direct_scale[None, :, None] * xs_f) * jax.nn.silu(output_gate_logits.astype(jnp.float32)).reshape(SEQ, HEADS, HEAD_DIM)
    gated = gated * lax.rsqrt(lax.optimization_barrier(jnp.mean(gated * gated, axis=-1, keepdims=True)) + eps)
    mixed = (gated.reshape(SEQ, INNER) * gated_norm_scale.astype(jnp.float32)).astype(jnp.bfloat16)
    mixer_out = jnp.dot(mixed, mixer_output_weight, preferred_element_type=jnp.float32).astype(jnp.bfloat16)
    tokens_f = second_batch_tokens.astype(jnp.float32)
    normed = (tokens_f * lax.rsqrt(lax.optimization_barrier(jnp.mean(tokens_f * tokens_f, axis=-1, keepdims=True)) + eps) * pre_expert_norm_scale.astype(jnp.float32)).astype(jnp.bfloat16)
    group_logits = jnp.dot(normed, group_router_columns, preferred_element_type=jnp.float32)
    expert_logits = jnp.dot(normed, expert_router_columns, preferred_element_type=jnp.float32)
    weights = route_weights(group_logits, expert_logits, routes)
    block_routes = routes.reshape(N_EP, TOKB, 2)
    positions = jax.vmap(lambda rows: slot_positions(rows, EXPERTS))(block_routes)
    slots = (block_routes.reshape(N_EP, TOKB * 2) * CAP + positions).astype(jnp.int32)
    token_ids = jnp.repeat(jnp.arange(TOKB, dtype=jnp.int32), 2)
    source = jnp.full((N_EP, EXPERTS * CAP), TOKB, jnp.int32)
    source = jax.vmap(lambda row, slot: row.at[slot].set(token_ids))(source, slots)
    padded = jnp.concatenate([normed.reshape(N_EP, TOKB, D), jnp.zeros((N_EP, 1, D), jnp.bfloat16)], axis=1)
    dispatched = jax.vmap(lambda rows, index: jnp.take(rows, index, axis=0))(padded, source)
    per_expert = jnp.transpose(dispatched.reshape(N_EP, EXPERTS, CAP, D), (1, 0, 2, 3)).reshape(EXPERTS, N_EP * CAP, D)
    outputs = lax.map(expert_apply, (per_expert, expert_gate_weight, expert_up_weight, expert_down_weight))
    by_source = jnp.transpose(outputs.reshape(EXPERTS, N_EP, CAP, D), (1, 0, 2, 3)).reshape(N_EP, EXPERTS * CAP, D)
    picked = jax.vmap(lambda rows, index: jnp.take(rows, index, axis=0))(by_source, slots).astype(jnp.float32)
    combined = lax.optimization_barrier(jnp.sum(picked.reshape(N_EP, TOKB, 2, D) * weights.reshape(N_EP, TOKB, 2, 1), axis=2))
    experts_out = combined.reshape(TOKENS, D).astype(jnp.bfloat16)
    return (mixer_out, experts_out)
```

```python
import functools

import jax
import jax.numpy as jnp
from jax import lax
from jax.experimental import pallas as pl
from jax.experimental.pallas import tpu as pltpu
from jax.sharding import PartitionSpec as P


HEADS = 32
STATE = 64
GROUPS = 4
BLOCK = 128
CORES = 2

eps = 1e-06
exact_prec = lax.Precision.HIGHEST
bf16 = jnp.bfloat16
f32 = jnp.float32

MIB = 1024 * 1024


def exchange(value, axis, flip):
    count = lax.axis_size(axis)
    return lax.ppermute(value, axis, [(i, i ^ flip) for i in range(count)])


def from_behind(value, axis, steps):
    count = lax.axis_size(axis)
    return lax.ppermute(value, axis, [(i, i + steps) for i in range(count - steps)])


def spread(value):
    count = lax.axis_size("ep")
    if count != 4:
        return [[exchange(value, "ep", k)] for k in range(1, count)]
    x, y = exchange(value, "ep", 1), exchange(value, "ep", 2)
    middle = value.shape[0] // 2
    top = exchange(y[:middle], "ep", 1)
    low = exchange(x[middle:], "ep", 2)
    return [[x], [y], [top, low]]


def swap_all(groups):
    out, n = [], 0
    for group in groups:
        row = []
        for value in group:
            n += 1
            row.append(exchange(value, "tp", 1))
        out.append(row)
    return out


def cut(refs, groups):
    out, at = [], 0
    for group in groups:
        out.append(refs[at : at + group])
        at += group
    return out, refs[at:]


def whole(shape):
    return pl.BlockSpec(shape, lambda *_: (0,) * len(shape))


def silu(v):
    return v / (1.0 + jnp.exp(-v))


def mm(a, b, precision=None):
    return jnp.dot(a, b, preferred_element_type=f32, precision=precision)


def coords(place, n_tp):
    t = place % n_tp
    return place // n_tp, t // CORES, t % CORES, t


def state_kernel(
    place_ref, rate_ref, x_ref, b_ref, c_ref, before_ref, x_taps_ref, b_taps_ref, c_taps_ref,
    logit_ref, extra_ref, normed_ref, routes_ref, groups_ref, experts_ref, xs_ref, cbs_ref, bt_ref, dt_ref, cum_ref, local_ref, total_ref,
    logits, extras, gain, *, n_tp,
):
    heads = logit_ref.shape[0]
    length, width = x_ref.shape
    nblk = length // BLOCK
    rows = nblk * 8
    pairs = heads // 2
    logits[...] = jnp.zeros(logits.shape, f32)
    extras[...] = jnp.zeros(extras.shape, f32)
    for b in range(nblk):
        logits[b * 8 : b * 8 + heads, :] = logit_ref[:, b * BLOCK : (b + 1) * BLOCK]
        extras[b * 8 : b * 8 + heads, :] = extra_ref[:, b * BLOCK : (b + 1) * BLOCK]
    head_row = lax.broadcasted_iota(jnp.int32, (8, BLOCK), 0)
    rate = jnp.zeros((8, BLOCK), f32)
    for h in range(heads):
        rate = jnp.where(head_row == h, rate_ref[h], rate)
    rate = jnp.concatenate([jnp.exp(rate)] * nblk, axis=0)
    v = logits[...]
    dt = jnp.maximum(v, 0.0) + jnp.log(1.0 + jnp.exp(-jnp.abs(v)))
    log_decay = extras[...] - dt * rate
    r0 = lax.broadcasted_iota(jnp.int32, (BLOCK, BLOCK), 0)
    r1 = lax.broadcasted_iota(jnp.int32, (BLOCK, BLOCK), 1)
    cum = mm(log_decay, (r0 <= r1).astype(f32), exact_prec)
    block_log = jnp.broadcast_to(cum[:, BLOCK - 1 :], (rows, BLOCK))
    q0 = lax.broadcasted_iota(jnp.int32, (rows, rows), 0)
    q1 = lax.broadcasted_iota(jnp.int32, (rows, rows), 1)
    same = (q0 % 8) == (q1 % 8)
    start = mm((same & (q1 // 8 < q0 // 8)).astype(f32), block_log, exact_prec)
    total = start + block_log
    dt_ref[...] = dt
    cum_ref[...] = cum
    gain[0] = dt * jnp.exp(block_log - cum)
    gain[1] = jnp.exp(block_log)
    gain[2] = start
    first = lax.broadcasted_iota(jnp.int32, (1, BLOCK), 1) < BLOCK // 2
    group = place_ref[0] % n_tp * heads // (HEADS // GROUPS)
    pair_at = pl.multiple_of(group // 2 * BLOCK, BLOCK)
    odd = group % 2 == 1

    def choose(c, b):
        c, b = c.astype(f32), b.astype(f32)
        c = jnp.where(odd, pltpu.roll(c, STATE, 1), c)
        b = jnp.where(odd, b, pltpu.roll(b, STATE, 1))
        return jnp.where(first, c, b)

    of_group = (slice(None), pl.ds(pair_at, BLOCK))
    cb_taps = choose(c_taps_ref[of_group], b_taps_ref[of_group])
    taps = jnp.concatenate([x_taps_ref[...].astype(f32), cb_taps], axis=1)

    def one(b, carry):
        tail, states = carry
        at = pl.multiple_of(b * BLOCK, BLOCK)
        x = x_ref[pl.ds(at, BLOCK), :].astype(f32)
        of_block = (pl.ds(at, BLOCK), pl.ds(pair_at, BLOCK))
        cb = choose(c_ref[of_block], b_ref[of_block])
        joined = jnp.concatenate([x, cb], axis=1)
        padded = jnp.concatenate([tail, joined], axis=0)
        conv = jnp.zeros(joined.shape, f32)
        n_taps = taps.shape[0]
        for j in range(n_taps):
            lo = 8 - (n_taps - 1) + j
            conv = conv + taps[j : j + 1] * padded[lo : lo + BLOCK]
        conv = silu(conv).astype(bf16)
        xs = conv[:, :width]
        xs_ref[pl.ds(at, BLOCK), :] = xs
        cbs_ref[pl.ds(at, BLOCK), :] = conv[:, width:]
        turned = jnp.transpose(conv[:, width:].astype(f32))
        bt = turned[STATE:]
        bt_ref[pl.ds(pl.multiple_of(b * STATE, STATE), STATE), :] = bt.astype(bf16)
        row = pl.multiple_of(b * 8, 8)
        factor = gain[0, pl.ds(row, 8), :]
        decay = gain[1, pl.ds(row, 8), :]
        begun = gain[2, pl.ds(row, 8), :]
        new = []
        for q in range(pairs):
            lanes = slice(q * BLOCK, (q + 1) * BLOCK)
            h = 2 * q
            local_ref[b, :STATE, lanes] = states[q]
            both = jnp.where(first, begun[h : h + 1], begun[h + 1 : h + 2])
            local_ref[b, STATE:, lanes] = jnp.broadcast_to(both, (8, BLOCK))
            left = jnp.concatenate(
                [bt * factor[h : h + 1], bt * factor[h + 1 : h + 2]], axis=0
            ).astype(bf16)
            added = mm(left, xs[:, lanes])
            added = jnp.where(first, added[:STATE], added[STATE:])
            keep = jnp.where(first, decay[h : h + 1], decay[h + 1 : h + 2])
            new.append(states[q] * keep + added)
        return joined[BLOCK - 8 :], tuple(new)

    maps = b_ref.shape[1]
    before_x = before_ref[:, :width]
    before_b = before_ref[:, pl.ds(pl.multiple_of(width + pair_at, BLOCK), BLOCK)]
    before_c = before_ref[:, pl.ds(pl.multiple_of(width + maps + pair_at, BLOCK), BLOCK)]
    tail = jnp.concatenate([before_x.astype(f32), choose(before_c, before_b)], axis=1)
    tail = tail[before_ref.shape[0] - 8 :]
    states = tuple(jnp.zeros((STATE, BLOCK), f32) for _ in range(pairs))
    _, states = lax.fori_loop(0, nblk, one, (tail, states))
    last = total[rows - 8 :]
    for q in range(pairs):
        lanes = slice(q * BLOCK, (q + 1) * BLOCK)
        total_ref[:STATE, lanes] = states[q]
        both = jnp.where(first, last[2 * q : 2 * q + 1], last[2 * q + 1 : 2 * q + 2])
        total_ref[STATE : STATE + 8, lanes] = jnp.broadcast_to(both, (8, BLOCK))
    n_tok = normed_ref.shape[0]
    weights = route_weights(normed_ref[...], groups_ref[...], experts_ref[...], routes_ref[...])
    for i, row in enumerate(weights):
        total_ref[STATE + 8 + i : STATE + 9 + i, :n_tok] = row


def route_weights(normed, groups, experts, routes):
    def log_softmax(rows):
        top = functools.reduce(jnp.maximum, rows)
        less = [row - top for row in rows]
        log_sum = jnp.log(sum(jnp.exp(row) for row in less))
        return [row - log_sum for row in less]

    def logits(columns):
        both = (((1,), (1,)), ((), ()))
        out = lax.dot_general(columns, normed, both, preferred_element_type=f32)
        return [out[i : i + 1] for i in range(out.shape[0])]

    group_lp, expert_rows = log_softmax(logits(groups)), logits(experts)
    n_experts = len(expert_rows)
    per_group = n_experts // len(group_lp)
    log_prob = []
    for g, lp in enumerate(group_lp):
        inner = log_softmax(expert_rows[g * per_group : (g + 1) * per_group])
        log_prob += [lp + row for row in inner]
    picks = [[routes[k : k + 1] == i for i in range(n_experts)] for k in range(routes.shape[0])]
    chosen = [sum(jnp.where(p, lp, 0.0) for p, lp in zip(pick, log_prob)) for pick in picks]
    top = functools.reduce(jnp.maximum, chosen)
    powers = [jnp.exp(c - top) for c in chosen]
    total = sum(powers)
    shares = [p / total for p in powers]
    return [
        sum(jnp.where(pick[i], share, 0.0) for pick, share in zip(picks, shares))
        for i in range(n_experts)
    ]


def mixed_kernel(
    place_ref, direct_ref, xs_ref, cbs_ref, bt_ref, dt_ref, cum_ref, local_ref, enter_ref,
    gate_ref, scale_ref, *out_refs,
):
    width = xs_ref.shape[1]
    first = lax.broadcasted_iota(jnp.int32, (1, BLOCK), 1) < BLOCK // 2
    r0 = lax.broadcasted_iota(jnp.int32, (BLOCK, BLOCK), 0)
    r1 = lax.broadcasted_iota(jnp.int32, (BLOCK, BLOCK), 1)
    lower = r0 >= r1
    mean_of = jnp.where((r0 // STATE) == (r1 // STATE), 1.0 / STATE, 0.0).astype(bf16)
    out = []
    for b in range(xs_ref.shape[0] // BLOCK):
        at = slice(b * BLOCK, (b + 1) * BLOCK)
        c = cbs_ref[at, :STATE]
        scores = mm(c, bt_ref[b * STATE : (b + 1) * STATE])
        cum = cum_ref[b * 8 : (b + 1) * 8]
        turned = jnp.transpose(cum)
        dt = dt_ref[b * 8 : (b + 1) * 8]
        row = []
        for q in range(width // BLOCK):
            lanes = slice(q * BLOCK, (q + 1) * BLOCK)
            left, columns = [], []
            for h in (2 * q, 2 * q + 1):
                column = jnp.broadcast_to(turned[:, h : h + 1], (BLOCK, BLOCK))
                decay = jnp.exp(jnp.where(lower, column - cum[h : h + 1], -jnp.inf))
                left.append((scores * decay * dt[h : h + 1]).astype(bf16))
                columns.append(column)
            xs = xs_ref[at, lanes]
            inner = mm(jnp.concatenate(left, axis=0), xs)
            inner = jnp.where(first, inner[:BLOCK], inner[BLOCK:])
            begun = local_ref[b, STATE : STATE + 1, lanes]
            state = local_ref[b, :STATE, lanes] + jnp.exp(begun) * enter_ref[:, lanes]
            high = state.astype(bf16)
            low = (state - high.astype(f32)).astype(bf16)
            carried = mm(c, high) + mm(c, low)
            ssm = inner + carried * jnp.exp(jnp.where(first, columns[0], columns[1]))
            gate = gate_ref[at, lanes].astype(f32)
            direct = jnp.where(first, direct_ref[2 * q], direct_ref[2 * q + 1])
            gated = (ssm + direct * xs.astype(f32)) * silu(gate)
            square = gated * gated
            high = square.astype(bf16)
            low = (square - high.astype(f32)).astype(bf16)
            mean = mm(high, mean_of) + mm(low, mean_of)
            gated = gated * lax.rsqrt(mean + eps) * scale_ref[:, lanes].astype(f32)
            row.append(gated.astype(bf16))
        out.append(jnp.concatenate(row, axis=1))
    out = jnp.concatenate(out, axis=0)
    for i, ref in enumerate(out_refs):

        @pl.when(pl.program_id(0) == i)
        def _(ref=ref):
            ref[...] = out


def project_kernel(place_ref, *refs, n_ep, n_z, chunks):
    pieces, refs = refs[: n_z * CORES], refs[n_z * CORES :]
    own_w, other_w = refs[:2]
    same, refs = cut(refs[2:], chunks)
    crossed, (out_ref, acc) = cut(refs, chunks)
    e, _, core, _ = coords(place_ref[0], n_z * CORES)
    slot = same[0][0].shape[1]
    near = jnp.concatenate([p[...] for p in pieces[:CORES]], axis=1)
    acc[...] = mm(near, jnp.concatenate([own_w[...], other_w[...]], axis=0))
    far = jnp.concatenate([p[...] for p in pieces[CORES:]], axis=1)
    turned = []
    for z in range(1, n_z):
        turned += [pieces[CORES * z + 1][...], pieces[CORES * z][...]]
    turned = jnp.concatenate(turned, axis=1)
    for k in range(n_ep):
        for left, right, c in ((far, same[k], core), (turned, crossed[k], 1 - core)):
            at = pl.multiple_of((CORES * (e ^ k) + c) * slot, slot)
            part = acc[:, pl.ds(at, slot)]
            size = left.shape[1] // len(right)
            for i, chunk in enumerate(right):
                part = part + mm(left[:, i * size : (i + 1) * size], chunk[...])
            out_ref[:, pl.ds(at, slot)] = part.astype(bf16)


def call(kernel, out_shape, vmem, **kw):
    return pl.pallas_call(
        kernel,
        out_shape=out_shape,
        compiler_params=pltpu.CompilerParams(vmem_limit_bytes=vmem * MIB),
        **kw,
    )


def mixed_calls(n_z):
    flips = list(range(n_z))[::-1]
    return [flips[: n_z // 2], flips[n_z // 2 :]]


def slotted(columns, n_ep):
    return columns // (n_ep * CORES) % BLOCK == 0


def norm_kernel(
    place_ref, tokens_ref, scale_ref, x_ref, b_ref, c_ref, normed_ref, half_ref, tail_ref, *, n_tp
):
    tail_ref[...] = jnp.concatenate([x_ref[...], b_ref[...], c_ref[...]], axis=1)
    tokens = tokens_ref[...].astype(f32)
    mean = jnp.mean(tokens * tokens, axis=-1, keepdims=True)
    scale = scale_ref[...].astype(f32)
    normed_ref[...] = (tokens * lax.rsqrt(mean + eps) * scale).astype(bf16)
    half = half_ref.shape[0]
    core = coords(place_ref[0], n_tp)[2]
    half_ref[...] = normed_ref[pl.ds(pl.multiple_of(core * half, half), half), :]


def hidden_kernel(place_ref, own_ref, *refs, n_ep, n_tp, chunks):
    mine, refs = cut(refs, chunks)
    other, refs = cut(refs, chunks)
    weights, refs = refs[:n_ep], refs[n_ep:]
    gate_ref, up_ref, out_ref, rows = refs
    e, _, core, _ = coords(place_ref[0], n_tp)
    n_tok = own_ref.shape[0]
    half = n_tok // CORES

    @pl.when(pl.program_id(0) == 0)
    def _():
        rows[:n_tok, :] = own_ref[...]
        for k in range(1, n_ep):
            for sources, c in ((mine[k - 1], core), (other[k - 1], 1 - core)):
                size = half // len(sources)
                for i, source in enumerate(sources):
                    at = pl.multiple_of(k * n_tok + c * half + i * size, size)
                    rows[pl.ds(at, size), :] = source[...]

    gate = mm(rows[...], gate_ref[0])
    upper = mm(rows[...], up_ref[0])
    for k in range(n_ep):
        at = slice(k * n_tok, (k + 1) * n_tok)
        row = jnp.broadcast_to(weights[k][pl.ds(STATE + 8 + e, 1), :n_tok], (8, n_tok))
        column = jnp.transpose(row)[:, :1]
        out_ref[at, :] = (silu(gate[at]) * upper[at] * column).astype(bf16)


def away_kernel(place_ref, hidden_ref, down_ref, out_ref):
    out_ref[...] = mm(hidden_ref[...], down_ref[0]).astype(bf16)


def keep_kernel(place_ref, hidden_ref, down_ref, swapped_ref, *out_refs):
    total = mm(hidden_ref[...], down_ref[0]) + swapped_ref[...].astype(f32)
    n_tok = out_refs[0].shape[0]
    for k, ref in enumerate(out_refs):
        ref[...] = total[k * n_tok : (k + 1) * n_tok].astype(bf16)


def add_up(parts):
    total = parts[0].astype(f32)
    for part in parts[1:]:
        total = total + part.astype(f32)
    return total.astype(bf16)


def per_device(
    mixer_input_channels,
    output_gate_logits,
    head_group_input_map,
    head_group_output_map,
    input_channel_taps,
    input_map_taps,
    output_map_taps,
    step_logits,
    head_log_rate,
    extra_log_decay,
    head_direct_scale,
    gated_norm_scale,
    mixer_output_weight,
    second_batch_tokens,
    pre_expert_norm_scale,
    group_router_columns,
    expert_router_columns,
    routes,
    expert_gate_weight,
    expert_up_weight,
    expert_down_weight,
):
    n_ep, n_tp = lax.axis_size("ep"), lax.axis_size("tp")
    n_z = n_tp // CORES
    e, t = lax.axis_index("ep"), lax.axis_index("tp")
    core = t % CORES
    length, width = mixer_input_channels.shape
    nblk = length // BLOCK
    place = (e * n_tp + t).astype(jnp.int32)[None]
    vmem = pl.BlockSpec(memory_space=pltpu.VMEM)
    smem = pl.BlockSpec(memory_space=pltpu.SMEM)

    tails = (mixer_input_channels, head_group_input_map, head_group_output_map)
    n_tail = sum(a.shape[1] for a in tails)
    n_tok, d = second_batch_tokens.shape
    half = n_tok // CORES
    normed, sent, last_rows = call(
        functools.partial(norm_kernel, n_tp=n_tp),
        [
            jax.ShapeDtypeStruct((n_tok, d), bf16),
            jax.ShapeDtypeStruct((half, d), bf16),
            jax.ShapeDtypeStruct((16, n_tail), bf16),
        ],
        60,
        grid=(1,),
        in_specs=[smem, whole((n_tok, d)), whole((1, d))]
        + [pl.BlockSpec((16, a.shape[1]), lambda g: (length // 16 - 1, 0)) for a in tails],
        out_specs=[whole((n_tok, d)), whole((half, d)), whole((16, n_tail))],
    )(place, second_batch_tokens, pre_expert_norm_scale[None], *tails)
    before = from_behind(last_rows, "ep", 1)
    mine = spread(sent)
    other = swap_all(mine)
    chunks = [len(m) for m in mine]

    other_w = exchange(mixer_output_weight, "tp", 1)
    w_cols = mixer_output_weight.shape[1]
    slot = w_cols // (n_ep * CORES)
    by_slot = slotted(w_cols, n_ep)
    if by_slot:
        at = (e * CORES + core) * slot
        start_w = jnp.concatenate(
            [
                lax.dynamic_slice_in_dim(mixer_output_weight, at, slot, 1),
                lax.dynamic_slice_in_dim(other_w, at, slot, 1),
            ],
            axis=0,
        )
        line = [exchange(start_w, "tp", CORES * k) for k in range(1, n_z)]
        line = jnp.concatenate(line, axis=0)
        same = [[line]] + spread(line)
        crossed = swap_all(same)

    rows = nblk * 8
    told_rows = STATE + 8 + -(-expert_router_columns.shape[1] // 8) * 8
    shapes = [
        jax.ShapeDtypeStruct((length, width), bf16),
        jax.ShapeDtypeStruct((length, 2 * STATE), bf16),
        jax.ShapeDtypeStruct((nblk * STATE, BLOCK), bf16),
        jax.ShapeDtypeStruct((rows, BLOCK), f32),
        jax.ShapeDtypeStruct((rows, BLOCK), f32),
        jax.ShapeDtypeStruct((nblk, STATE + 8, width), f32),
        jax.ShapeDtypeStruct((told_rows, max(width, n_tok)), f32),
    ]
    xs, cbs, bt, dt, cum, local, own = call(
        functools.partial(state_kernel, n_tp=n_tp),
        shapes,
        60,
        in_specs=[smem] * 2 + [vmem] * 13,
        out_specs=[vmem] * 7,
        scratch_shapes=[
            pltpu.VMEM((rows, BLOCK), f32),
            pltpu.VMEM((rows, BLOCK), f32),
            pltpu.VMEM((3, rows, BLOCK), f32),
        ],
    )(
        place,
        head_log_rate,
        mixer_input_channels,
        head_group_input_map,
        head_group_output_map,
        before,
        input_channel_taps,
        input_map_taps,
        output_map_taps,
        step_logits,
        extra_log_decay,
        normed,
        routes.T,
        group_router_columns.T,
        expert_router_columns.T,
    )
    reached = {k: exchange(own, "ep", k) for k in range(1, n_ep)}
    entering = jnp.zeros((STATE, width), f32)
    for k, value in reached.items():
        between = jnp.zeros((1, width), f32)
        for k2, value2 in reached.items():
            inside = ((e ^ k) < (e ^ k2)) & ((e ^ k2) < e)
            between = between + jnp.where(inside, value2[STATE : STATE + 1, :width], 0.0)
        entered = value[:STATE, :width] * jnp.exp(between)
        entering = entering + jnp.where((e ^ k) < e, entered, 0.0)

    out_rows = length // n_tp
    per_piece = out_rows // BLOCK
    scale = gated_norm_scale[None]

    def mixed_for(flips):
        def by_row(shape):
            def at(g, p):
                flip = flips[0] * CORES + g
                for i in range(1, len(flips)):
                    flip = jnp.where(g >= i * CORES, flips[i] * CORES + g - i * CORES, flip)
                return (p[0] % n_tp ^ flip,) + (0,) * (len(shape) - 1)

            return pl.BlockSpec(shape, at)

        n_out = CORES * len(flips)
        return call(
            mixed_kernel,
            [jax.ShapeDtypeStruct((out_rows, width), bf16)] * n_out,
            16,
            grid_spec=pltpu.PrefetchScalarGridSpec(
                num_scalar_prefetch=1,
                grid=(n_out,),
                in_specs=[
                    smem,
                    by_row((out_rows, width)),
                    by_row((out_rows, 2 * STATE)),
                    by_row((per_piece * STATE, BLOCK)),
                    by_row((per_piece * 8, BLOCK)),
                    by_row((per_piece * 8, BLOCK)),
                    by_row((per_piece, STATE + 8, width)),
                    whole((STATE, width)),
                    by_row((out_rows, width)),
                    whole((1, width)),
                ],
                out_specs=[whole((out_rows, width))] * n_out,
            ),
        )(
            place,
            head_direct_scale,
            xs,
            cbs,
            bt,
            dt,
            cum,
            local,
            entering,
            output_gate_logits,
            scale,
        )

    pieces = {}
    for flips in mixed_calls(n_z):
        ats = [CORES * flip + i for flip in flips for i in range(CORES)]
        for at, piece in zip(ats, mixed_for(flips)):
            pieces[at] = exchange(piece, "tp", at) if at else piece
    pieces = [pieces[at] for at in range(n_tp)]

    ff = expert_gate_weight.shape[2]
    tile = min(ff, 256)
    hidden = call(
        functools.partial(hidden_kernel, n_ep=n_ep, n_tp=n_tp, chunks=chunks),
        jax.ShapeDtypeStruct((n_ep * n_tok, ff), bf16),
        60 if n_ep > 4 else 24,
        grid_spec=pltpu.PrefetchScalarGridSpec(
            num_scalar_prefetch=1,
            grid=(ff // tile,),
            in_specs=[whole((n_tok, d))]
            + [whole(m.shape) for m in sum(mine + other, [])]
            + [whole(own.shape)] * n_ep
            + [pl.BlockSpec((1, d, tile), lambda g, p: (0, 0, g))] * 2,
            out_specs=pl.BlockSpec((n_ep * n_tok, tile), lambda g, p: (0, g)),
            scratch_shapes=[pltpu.VMEM((n_ep * n_tok, d), bf16)],
        ),
    )(
        place,
        normed,
        *sum(mine + other, []),
        own,
        *[reached[k] for k in range(1, n_ep)],
        expert_gate_weight,
        expert_up_weight,
    )

    feats = d // n_tp

    def down_spec(away):
        def at(g, p):
            _, z, c, _ = coords(p[0], n_tp)
            return 0, 0, CORES * (z ^ g) + (1 - c if away else c)

        return pl.BlockSpec((1, ff, feats), at)

    all_rows = pl.BlockSpec((n_ep * n_tok, feats), lambda g, p: (0, g))
    away = call(
        away_kernel,
        jax.ShapeDtypeStruct((n_ep * n_tok, n_z * feats), bf16),
        12 if n_ep <= 4 else 40,
        grid_spec=pltpu.PrefetchScalarGridSpec(
            num_scalar_prefetch=1,
            grid=(n_z,),
            in_specs=[whole((n_ep * n_tok, ff)), down_spec(True)],
            out_specs=all_rows,
        ),
    )(place, hidden, expert_down_weight)
    swapped = exchange(away, "tp", 1)
    kept = call(
        keep_kernel,
        [jax.ShapeDtypeStruct((n_tok, n_z * feats), bf16)] * n_ep,
        16 if n_ep <= 4 else 40,
        grid_spec=pltpu.PrefetchScalarGridSpec(
            num_scalar_prefetch=1,
            grid=(n_z,),
            in_specs=[whole((n_ep * n_tok, ff)), down_spec(False), all_rows],
            out_specs=[pl.BlockSpec((n_tok, feats), lambda g, p: (0, g))] * n_ep,
        ),
    )(place, hidden, expert_down_weight, swapped)
    parts = [kept[0]] + [exchange(kept[k], "ep", k) for k in range(1, n_ep)]
    line_sum = []
    for k in range(n_z):
        line_sum.append(add_up([p[:, k * feats : (k + 1) * feats] for p in parts]))
    last = [line_sum[0]] + [exchange(line_sum[k], "tp", CORES * k) for k in range(1, n_z)]
    experts_out = add_up(last)

    if by_slot:
        mixer_out = call(
            functools.partial(
                project_kernel, n_ep=n_ep, n_z=n_z, chunks=[len(group) for group in same]
            ),
            jax.ShapeDtypeStruct((out_rows, w_cols), bf16),
            20,
            in_specs=[smem] + [vmem] * (n_tp + 2 + 2 * len(sum(same, []))),
            out_specs=vmem,
            scratch_shapes=[pltpu.VMEM((out_rows, w_cols), f32)],
        )(place, *pieces, mixer_output_weight, other_w, *sum(same + crossed, []))
    else:
        gathered = lax.all_gather(mixer_output_weight, "tp", axis=0)
        total = jnp.zeros((out_rows, w_cols), f32)
        for at in range(n_tp):
            w = lax.dynamic_index_in_dim(gathered, t ^ at, 0, False)
            total = total + jnp.dot(pieces[at], w, preferred_element_type=f32)
        mixer_out = total.astype(bf16)
    return (mixer_out, experts_out)


def solution(mesh):
    in_specs = (
        P("ep", "tp"),
        P("ep", "tp"),
        P("ep", None),
        P("ep", None),
        P(None, "tp"),
        P(),
        P(),
        P("tp", "ep"),
        P("tp"),
        P("tp", "ep"),
        P("tp"),
        P("tp"),
        P("tp", None),
        P("ep", None),
        P(),
        P(),
        P(),
        P("ep", None),
        P("ep", None, "tp"),
        P("ep", None, "tp"),
        P("ep", "tp", None),
    )
    out_specs = (P(("ep", "tp"), None), P("ep", "tp"))

    return jax.shard_map(
        per_device, mesh=mesh, in_specs=in_specs, out_specs=out_specs, check_vma=False
    )
```
